256 devices in a mesh: grp: 2 (over y), fs: 16 (over z), tp: 8 (over x, core).
Axes of the slice: x: 4, y: 2, z: 16, core: 2. Of those that a mesh axis runs over, the one named last changes fastest.
The devices are a block of a 4x16x16 slice.
Arguments:
- tokens: bfloat16 [4096, 4096], P(('grp', 'tp')), parts along dimension 0, may hold values from -6 to 6
- routes: int32 [4096, 2], P(('grp', 'tp')), parts along dimension 0, may hold values from 0 to 7, all different within a row; in each aligned block of 256 rows (0 to 255, 256 to 511, ...) at most 128 rows name the same one
- route_weight: float32 [4096, 2], P(('grp', 'tp')), parts along dimension 0, may hold values from 0.2 to 1
- norm_gain: float32 [4096], P('fs'), may hold values from 0.1 to 1.9
- gate_train: float32 [8, 4096, 2048], P(None, 'fs', 'tp'), may hold values from -0.09375 to 0.09375
- up_train: float32 [8, 4096, 2048], P(None, 'fs', 'tp'), may hold values from -0.09375 to 0.09375
- down_train: float32 [8, 2048, 4096], P(None, 'fs', 'tp'), may hold values from -0.125 to 0.125
Outputs:
- gate_serve: bfloat16 [16, 4096, 2048], P(('grp', 'tp'), None, 'fs'), parts along dimension 0
- up_serve: bfloat16 [16, 4096, 2048], P(('grp', 'tp'), None, 'fs'), parts along dimension 0
- down_serve: bfloat16 [16, 2048, 4096], P(('grp', 'tp'), 'fs'), parts along dimension 0
- moe_out: bfloat16 [4096, 4096], P(('grp', 'tp'), 'fs'), parts along dimension 0
The draws below stay inside these ranges and needn't reach their ends.
There are 2 independent parts, one for each index of `grp`. The reference program is written for one: setup_inputs(seed, part) draws one part's arguments, and reference() takes and returns one part's arrays. A program takes and returns all parts, laid end to end along the dimension named above; an argument that names none is the same for every part. Nothing has to cross between parts.
Inputs may be any that keep to these rules, and one draw needn't show every extreme that they name: `routes`: within the 256 rows of each device (aligned blocks), no expert is named by more than 128 rows, a bound that some block reaches; the two experts of a row differ; every expert is named somewhere.
All inputs are finite; a program needn't handle non-finite values.
Results may differ from the reference program's by a relative error of at most 0.0076.
Values may be sent and summed in bfloat16 or wider, within the bound.
No kernel may reach another device: no remote copies, remote signals or barrier semaphores. Data moves between devices by JAX's collectives and lax.ppermute only.
A program may use at most 128 MiB of HBM per device.

```python
import math
import jax
import jax.numpy as jnp
import numpy as np
from jax import lax

D = 4096
FF = 2048
EXPERTS = 8
TOK_DEV = 256
CAP = 128
TOKENS = 2048


def block_scale(stream_key, shape, pieces, low, high):
    def one(axis_at, shards_of):
        steps = jax.random.uniform(jax.random.fold_in(jax.random.fold_in(stream_key, 6), axis_at), (shards_of,), jnp.float32, low / len(pieces), high / len(pieces))
        return jnp.repeat(jnp.exp(steps), shape[axis_at] // shards_of).reshape((-1,) + (1,) * (len(shape) - axis_at - 1))

    level = one(*pieces[0])
    for cut in pieces[1:]:
        level = level * one(*cut)
    return level


def routed_block(own_key, own, number, rows, number_of, top, reach, skew):
    order = jax.random.permutation(own_key, number_of)
    crowded, common = shares(number_of, rows * top, reach, skew, True), shares(number_of, rows * top, reach, skew, False)
    places = jnp.arange(number_of)

    def named(sizes, offset_by):
        used = int((sizes > 0).sum())
        fixed = max(1, used // 4)
        passed = fixed + (places - fixed + offset_by * (used - fixed)) % max(1, number_of - fixed)
        return jnp.zeros((number_of,), jnp.int32).at[order[jnp.where(places < fixed, places, passed)]].set(jnp.asarray(sizes, jnp.int32))

    sizes = jnp.where(number % 4 == 0, named(crowded, number // 4), named(common, number - number // 4 - 1))
    mixed = jax.random.permutation(jax.random.fold_in(own, 3), number_of)
    giver, taker = mixed[0:number_of // 2 * 2:2], mixed[1:number_of // 2 * 2:2]
    margin = jnp.minimum(sizes[giver] - 1, reach - sizes[taker]) // 2
    margin = jnp.where((giver == order[0]) | (taker == order[0]) | (sizes[taker] == 0), 0, jnp.maximum(margin, 0))
    passed = jax.random.randint(jax.random.fold_in(own, 4), (number_of // 2,), 0, 1 << 20) % (margin + 1)
    sizes = sizes.at[giver].add(-passed).at[taker].add(passed)
    items = jnp.searchsorted(jnp.cumsum(sizes), jnp.arange(rows * top), side="right").astype(jnp.int32)
    grid = items.reshape(top, rows).T
    grid = grid[jax.random.permutation(jax.random.fold_in(own, 1), rows)]
    offset_by = jax.random.randint(jax.random.fold_in(own, 2), (rows, 1), 0, top)
    return jnp.take_along_axis(grid, (jnp.arange(top)[None, :] + offset_by) % top, axis=1)


def shares(amount, total, reach, skew, full):
    weights = [(1 << 20) // math.isqrt(standing ** skew) + 1 for standing in range(1, amount + 1)]
    largest = reach if full else min(reach, max(-(-total // amount), total * weights[0] // sum(weights)))
    least = 1 if total - largest >= amount - 1 else 0
    counts, rest = [largest] + [least] * (amount - 1), total - largest - least * (amount - 1)
    while rest > 0:
        free = [i for i in range(1, amount) if counts[i] < largest] or [i for i in range(1, amount) if counts[i] < reach]
        mass, remaining = sum([weights[i] for i in free]), rest
        for i in free:
            addition = min(reach - counts[i], max(1, remaining * weights[i] // mass), rest)
            counts[i] = counts[i] + addition
            rest = rest - addition
    return np.array(counts)


def centred(rng, extent, scale, bound, split=(), kind=jnp.bfloat16):
    values = scale * jax.random.normal(rng, extent, jnp.float32)
    if split:
        values = values * block_scale(rng, extent, split, -0.22, 0.18)
    return jnp.clip(values, -bound, bound).astype(kind)


def setup_inputs(seed: int = 0, part: int = 0) -> dict:
    key_list = jax.random.split(jax.random.key(seed), 8)
    part_splits = jax.random.split(jax.random.fold_in(key_list[7], part), 8)
    tokens = centred(part_splits[0], (TOKENS, D), 1.0, 6.0, ((0, 8),))
    routes_keys = jax.random.split(jax.random.fold_in(part_splits[1], 1), TOKENS // TOK_DEV)
    routes_turns = jax.random.permutation(jax.random.fold_in(part_splits[1], 3), TOKENS // TOK_DEV)
    routes = jax.vmap(lambda own, number: routed_block(jax.random.fold_in(part_splits[1], 2), own, number, TOK_DEV, EXPERTS, 2, CAP, 1))(routes_keys, routes_turns).reshape((TOKENS, 2))
    route_weight = jnp.clip(0.2 + 0.8 * jax.random.uniform(part_splits[2], (TOKENS, 2), jnp.float32) ** block_scale(part_splits[2], (TOKENS, 2), ((0, 8),), -0.2, 0.2), 0.2, 1.0)
    norm_gain = jnp.clip(1.0 + 0.18 * jax.random.normal(key_list[3], (D,), jnp.float32), 0.1, 1.9)
    gate_train = centred(key_list[4], (EXPERTS, D, FF), D ** -0.5, 0.09375, ((1, 16), (2, 8)), jnp.float32)
    up_train = centred(key_list[5], (EXPERTS, D, FF), D ** -0.5, 0.09375, ((1, 16), (2, 8)), jnp.float32)
    down_train = centred(key_list[6], (EXPERTS, FF, D), FF ** -0.5, 0.125, ((1, 16), (2, 8)), jnp.float32)
    return {"tokens": tokens, "routes": routes, "route_weight": route_weight, "norm_gain": norm_gain, "gate_train": gate_train, "up_train": up_train, "down_train": down_train}


def reference(tokens, routes, route_weight, norm_gain, gate_train, up_train, down_train):
    gate_serve = (norm_gain[None, :, None] * gate_train).astype(jnp.bfloat16)
    up_serve = (norm_gain[None, :, None] * up_train).astype(jnp.bfloat16)
    down_serve = down_train.astype(jnp.bfloat16)

    def expert_step(total, inputs):
        index, gate_one, up_one, down_one = inputs
        gate_h = jnp.dot(tokens, gate_one, preferred_element_type=jnp.float32)
        up_h = jnp.dot(tokens, up_one, preferred_element_type=jnp.float32)
        hidden = (jax.nn.silu(gate_h) * up_h).astype(jnp.bfloat16)
        result = jnp.dot(hidden, down_one, preferred_element_type=jnp.float32).astype(jnp.bfloat16)
        result = lax.optimization_barrier(result)
        weight = jnp.sum(jnp.where(routes == index, route_weight, jnp.zeros_like(route_weight)), axis=1)
        return total + weight[:, None] * result.astype(jnp.float32), None

    start = jnp.zeros((tokens.shape[0], tokens.shape[1]), jnp.float32)
    total, _ = lax.scan(expert_step, start,
                        (jnp.arange(EXPERTS, dtype=jnp.int32), gate_serve, up_serve, down_serve))
    return gate_serve, up_serve, down_serve, total.astype(jnp.bfloat16)
```

```python
import functools

import jax
import jax.numpy as jnp
from jax import lax
from jax.experimental import pallas as pl
from jax.experimental.pallas import tpu as pltpu
from jax.sharding import PartitionSpec as P

CAP = 128
CORES = 2
BF16 = jnp.bfloat16
F32 = jnp.float32


def after(value, *others):
    return lax.optimization_barrier((value, *others))[0]


def exchange(value, axis):
    return lax.all_to_all(value, axis, split_axis=0, concat_axis=0, tiled=True)


def shared_by_groups(value):
    groups = lax.axis_size("grp")
    pieces, ahead, behind = [(0, value)], value, value
    for k in range(1, groups // 2 + 1):
        ahead = lax.ppermute(ahead, "grp", [(i, (i + 1) % groups) for i in range(groups)])
        pieces.append((-k, ahead))
        if 2 * k < groups:
            behind = lax.ppermute(behind, "grp", [(i, (i - 1) % groups) for i in range(groups)])
            pieces.append((k, behind))
    return pieces


def interleaved(pieces):
    groups = lax.axis_size("grp")
    mine = lax.axis_index("grp")
    own = pieces[0][1]
    if groups == 1:
        return own[:, None]
    if groups == 2:
        other = pieces[1][1]
        first = jnp.where(mine == 0, own, other)
        second = jnp.where(mine == 0, other, own)
        return jnp.stack([first, second], axis=1)
    full = jnp.zeros((own.shape[0], groups, *own.shape[1:]), own.dtype)
    for offset, piece in pieces:
        full = lax.dynamic_update_slice_in_dim(full, piece[:, None], (mine + offset) % groups, 1)
    return full


def chip_shift(tp, step, swap=False):
    chips = tp // CORES
    return [
        (CORES * x + c, CORES * ((x + step) % chips) + (1 - c if swap else c))
        for x in range(chips)
        for c in range(CORES)
    ]


def tokens_of_all(tokens):
    tp = lax.axis_size("tp")
    assert tp == 8
    half = tokens.shape[0] // 2
    from_left = lax.ppermute(tokens, "tp", chip_shift(tp, 1))
    from_right = lax.ppermute(tokens, "tp", chip_shift(tp, -1))
    opposite_a = lax.ppermute(from_left[:half], "tp", chip_shift(tp, 1))
    opposite_b = lax.ppermute(from_right[half:], "tp", chip_shift(tp, -1))
    swap = lambda v: lax.ppermute(v, "tp", chip_shift(tp, 0, True))
    return [
        (tokens,), (swap(tokens),),
        (from_right,), (swap(from_right),),
        (opposite_a, opposite_b), (swap(opposite_a), swap(opposite_b)),
        (from_left,), (swap(from_left),),
    ]


def hidden_kernel(layout, *refs):
    n = len(layout)
    toks = refs[:n]
    gate_ref, up_ref, slot_ref, out_ref, buf, weights, sems = refs[n:]
    rows, depth = buf.shape[1:]
    slots = buf.shape[0]

    def copy(i):
        block, row, length = layout[i]
        s = block % slots
        return pltpu.make_async_copy(toks[i], buf.at[s, pl.ds(row, length)], sems.at[i])

    blocks = layout[-1][0] + 1
    of = [[i for i in range(n) if layout[i][0] == b] for b in range(blocks)]
    for b in range(min(slots, blocks)):
        for i in of[b]:
            copy(i).start()
    width = gate_ref.shape[1]
    weights[:, :width] = gate_ref[...]
    weights[:, width:] = up_ref[...]
    for b in range(blocks):
        for i in of[b]:
            copy(i).wait()
        both = jnp.dot(buf[b % slots], weights[...], preferred_element_type=F32)
        gate, up = both[:, :width], both[:, width:]
        hid = (gate / (1.0 + jnp.exp(-gate)) * up).astype(BF16)
        at = lax.broadcasted_iota(jnp.int32, (CAP, rows), 0)
        pick = (at == slot_ref[b]).astype(BF16)
        out_ref[pl.ds(b * CAP, CAP), :] = jnp.dot(
            pick, hid, preferred_element_type=F32
        ).astype(BF16)
        if b + slots < blocks:
            for i in of[b + slots]:
                copy(i).start()


def hidden_of(blocks, gate, up, slots):
    rows, depth = blocks[0][0].shape
    layout, parts = [], []
    for b, pieces in enumerate(blocks):
        row = 0
        for piece in pieces:
            layout.append((b, row, piece.shape[0]))
            parts.append(piece)
            row += piece.shape[0]
    width = gate.shape[1]
    flops = 2 * len(blocks) * rows * depth * 2 * width
    return pl.pallas_call(
        functools.partial(hidden_kernel, layout),
        out_shape=jax.ShapeDtypeStruct((len(blocks) * CAP, width), BF16),
        in_specs=[pl.BlockSpec(memory_space=pl.ANY)] * len(parts)
        + [pl.BlockSpec(memory_space=pltpu.VMEM)] * 3,
        out_specs=pl.BlockSpec(memory_space=pltpu.VMEM),
        scratch_shapes=[
            pltpu.VMEM((4, rows, depth), BF16),
            pltpu.VMEM((depth, 2 * width), BF16),
            pltpu.SemaphoreType.DMA((len(parts),)),
        ],
        compiler_params=pltpu.CompilerParams(vmem_limit_bytes=40 * 2**20),
        cost_estimate=pl.CostEstimate(
            flops=flops, bytes_accessed=2 * len(blocks) * rows * depth, transcendentals=0
        ),
        name="hidden",
    )(*parts, gate, up, slots)


def pair_exchange(fs, tp, step):
    pairs = []
    for i in range(fs):
        for t in range(tp):
            c = t % CORES
            up = (i + step + c) % 2 == 0
            j = (i + 1) % fs if up else (i - 1) % fs
            pairs.append((i * tp + t, j * tp + t))
    return pairs


def per_device(tokens, routes, route_weight, norm_gain, gate_train, up_train, down_train):
    groups, fs, tp = (lax.axis_size(a) for a in ("grp", "fs", "tp"))
    grp_at, fs_at, tp_at = (lax.axis_index(a) for a in ("grp", "fs", "tp"))
    core, chip = tp_at % CORES, tp_at // CORES
    experts, d_rows, ff_cols = gate_train.shape
    f_rows, d_cols = down_train.shape[1:]
    assert experts == tp
    width = ff_cols * tp // fs
    out_cols = d_cols * tp // fs
    r, rd = d_rows // groups, f_rows // groups

    gain = lax.dynamic_slice_in_dim(norm_gain, grp_at * r, r, 0)

    def share(w):
        w = lax.dynamic_slice_in_dim(w, grp_at * r, r, 1)
        w = (gain[None, :, None] * w).astype(BF16)
        return jnp.swapaxes(w.reshape(experts, r, ff_cols // width, width), 1, 2)

    down = lax.dynamic_slice_in_dim(down_train, grp_at * rd, rd, 1).astype(BF16)
    lanes = out_cols // width
    down = down.reshape(experts, rd, d_cols // out_cols, lanes, width)
    down = jnp.moveaxis(down, 1, 3).reshape(experts, d_cols // out_cols, lanes * rd, width)
    both = jnp.concatenate([share(gate_train), share(up_train), down], axis=2)
    arrived = exchange(both, "tp").reshape(fs, both.shape[2], width)

    blocks = tokens_of_all(after(tokens, arrived))

    gate_z = exchange(arrived[:, :r], "fs")
    up_z = exchange(after(arrived[:, r : 2 * r], gate_z), "fs")
    down_m = arrived[:, 2 * r :]
    down_z = exchange(after(down_m, up_z), "fs")
    gate_serve = interleaved(shared_by_groups(gate_z)).reshape(fs * d_rows, width)
    up_serve = interleaved(shared_by_groups(up_z)).reshape(fs * d_rows, width)

    def down_whole(v):
        v = v.reshape(fs * lanes, rd, width)
        v = interleaved(shared_by_groups(v))
        return v.reshape(fs, lanes, f_rows, width)

    down_serve = jnp.transpose(down_whole(down_m), (2, 0, 1, 3)).reshape(f_rows, fs * out_cols)
    down_cols = jnp.transpose(down_whole(down_z), (0, 2, 1, 3)).reshape(fs, f_rows, out_cols)

    def slots_of(chosen, expert):
        named = jnp.any(chosen == expert, axis=-1)
        order = jnp.cumsum(named.astype(jnp.int32), axis=-1) - 1
        return jnp.where(named, order, -1)

    routes_all = lax.all_gather(routes, "tp", axis=0, tiled=False)
    chips = tp // CORES
    src = [
        CORES * ((chip + dx) % chips) + (core if dc == 0 else 1 - core)
        for dx in range(chips)
        for dc in range(CORES)
    ]
    slots_all = slots_of(routes_all, tp_at)
    slots = jnp.stack([lax.dynamic_index_in_dim(slots_all, s, 0) for s in src])

    hidden = hidden_of(blocks, gate_serve, up_serve, slots)

    count = hidden.shape[0]
    lower = (fs_at + core) % 2 == 0
    own_pair = ((fs_at - core) % fs) // 2
    down_rows = jnp.concatenate([down_cols, down_cols[:1]], axis=0)

    def down_pair(m):
        start = 2 * (m % (fs // 2)) + core
        rows = lax.dynamic_slice_in_dim(down_rows, start, 2, 0)
        return rows.reshape(2 * f_rows, out_cols)

    chunks = 2
    pieces = jnp.split(hidden, chunks, axis=0)
    totals = [None] * chunks
    current = [None] * chunks
    for step in range(fs // 2):
        perm = pair_exchange(fs, tp, step)
        for k in range(chunks):
            if step == 0:
                got = lax.ppermute(pieces[k], ("fs", "tp"), perm)
                current[k] = jnp.where(
                    lower,
                    jnp.concatenate([pieces[k], got], axis=1),
                    jnp.concatenate([got, pieces[k]], axis=1),
                )
            else:
                current[k] = lax.ppermute(current[k], ("fs", "tp"), perm)
        away = (step + 1) // 2 * (-1 if step % 2 else 1)
        m = jnp.where(lower, own_pair + away, own_pair - away)
        for k in range(chunks):
            term = jnp.dot(current[k], down_pair(m), preferred_element_type=F32)
            totals[k] = term if totals[k] is None else totals[k] + term
    result = jnp.concatenate([t.astype(BF16) for t in totals], axis=0)
    result = result.reshape(tp, CAP, out_cols)
    back = [
        CORES * ((p // CORES - chip) % chips) + (p % CORES + core) % CORES for p in range(tp)
    ]
    leaving = jnp.concatenate([lax.dynamic_slice_in_dim(result, b, 1, 0) for b in back], axis=0)
    returned = exchange(leaving, "tp").reshape(tp * CAP, out_cols)

    ids = jnp.arange(experts, dtype=jnp.int32)
    slot_of = slots_of(routes[None], ids[:, None, None])
    own_slot = jnp.sum(
        jnp.where(routes[:, :, None] == ids[None, None, :], slot_of.T[:, None, :], 0), axis=2
    )
    place = routes * CAP + own_slot
    at = jnp.arange(experts * CAP, dtype=jnp.int32)
    picked = [
        jnp.dot(
            (place[:, k, None] == at[None, :]).astype(BF16), returned, preferred_element_type=F32
        )
        for k in range(2)
    ]
    mixed = route_weight[:, :1] * picked[0] + route_weight[:, 1:] * picked[1]
    return gate_serve[None], up_serve[None], down_serve[None], mixed.astype(BF16)


def solution(mesh):
    return jax.shard_map(
        per_device,
        mesh=mesh,
        in_specs=(
            P(("grp", "tp"), None),
            P(("grp", "tp"), None),
            P(("grp", "tp"), None),
            P("fs"),
            P(None, "fs", "tp"),
            P(None, "fs", "tp"),
            P(None, "fs", "tp"),
        ),
        out_specs=(
            P(("grp", "tp"), None, "fs"),
            P(("grp", "tp"), None, "fs"),
            P(("grp", "tp"), "fs", None),
            P(("grp", "tp"), "fs"),
        ),
        check_vma=False,
    )
```
